256 devices in a mesh: ep: 64 (over z, y, core), tp: 4 (over x).
Axes of the slice: x: 4, y: 4, z: 8, core: 2. Of those that a mesh axis runs over, the one named last changes fastest.
Arguments:
- tokens: bfloat16 [14336, 2048], P('ep'), may hold values from -6 to 6
- cotangent: bfloat16 [14336, 2048], P('ep'), may hold values from -6 to 6
- routes: int32 [14336, 2], P('ep'), may hold values from 0 to 63, all different within a row; in each aligned block of 224 rows (0 to 223, 224 to 447, ...) at most 14 rows name the same one
- gate_weights: float32 [14336, 2], P('ep'), may hold values from 0.2 to 1
- w_gate: bfloat16 [64, 2048, 1792], P('ep', None, 'tp'), may hold values from -0.125 to 0.125
- w_up: bfloat16 [64, 2048, 1792], P('ep', None, 'tp'), may hold values from -0.125 to 0.125
- w_down: bfloat16 [64, 1792, 2048], P('ep', 'tp'), may hold values from -0.125 to 0.125
Outputs:
- token_grad: bfloat16 [14336, 2048], P('ep', 'tp')
- score_grad: float32 [14336, 2], P('ep')
- gate_grad: bfloat16 [64, 2048, 1792], P('ep', None, 'tp')
- up_grad: bfloat16 [64, 2048, 1792], P('ep', None, 'tp')
- down_grad: bfloat16 [64, 1792, 2048], P('ep', 'tp')
- row_norms: float32 [2048], replicated
The draws below stay inside these ranges and needn't reach their ends.
Inputs may be any that keep to these rules, and one draw needn't show every extreme that they name: `routes`: within the rows of one device, no expert is named by more than 14 of the pairs; some expert is named by exactly 14 of them in some blocks. The 2 experts of a token differ.
All inputs are finite; a program needn't handle non-finite values.
Results may differ from the reference program's by a relative error of at most 0.014.
Values may be sent and summed in bfloat16 or wider, within the bound.
No kernel may reach another device: no remote copies, remote signals or barrier semaphores. Data moves between devices by JAX's collectives and lax.ppermute only.
A program may use at most 128 MiB of HBM per device.

```python
import math
import jax
import jax.numpy as jnp
import numpy as np
from jax import lax

D = 2048
FF = 1792
TOP = 2
TOK_DEV = 224
EXPERTS = 64
CAP = 14
TOKENS = 14336
N_EP = 64
N_TP = 4


def steps_of(own_key, extent, cuts, low, high):
    level, own = 1.0, jax.random.fold_in(own_key, 6)
    for dim, shards_of in cuts:
        heights = jnp.exp(jax.random.uniform(jax.random.fold_in(own, dim), (shards_of,), jnp.float32, low / len(cuts), high / len(cuts)))
        level = level * jnp.repeat(heights, extent[dim] // shards_of).reshape([-1 if axis == dim else 1 for axis in range(len(extent))])
    return level


def routed_block(rng, own, number, rows, number_of, top, bound, slope):
    order = jax.random.permutation(rng, number_of)
    packed, usual = load_shares(number_of, rows * top, bound, slope, True), load_shares(number_of, rows * top, bound, slope, False)
    places = jnp.arange(number_of)

    def named(tallies, turn):
        used = int((tallies > 0).sum())
        fixed = max(1, used // 4)
        moved = fixed + (places - fixed + turn * (used - fixed)) % max(1, number_of - fixed)
        return jnp.zeros((number_of,), jnp.int32).at[order[jnp.where(places < fixed, places, moved)]].set(jnp.asarray(tallies, jnp.int32))

    tallies = jnp.where(number % 4 == 0, named(packed, number // 4), named(usual, number - number // 4 - 1))
    mixed = jax.random.permutation(jax.random.fold_in(own, 3), number_of)
    donor, sink = mixed[0:number_of // 2 * 2:2], mixed[1:number_of // 2 * 2:2]
    slack = jnp.minimum(tallies[donor] - 1, bound - tallies[sink]) // 2
    slack = jnp.where((donor == order[0]) | (sink == order[0]) | (tallies[sink] == 0), 0, jnp.maximum(slack, 0))
    moved = jax.random.randint(jax.random.fold_in(own, 4), (number_of // 2,), 0, 1 << 20) % (slack + 1)
    tallies = tallies.at[donor].add(-moved).at[sink].add(moved)
    items = jnp.searchsorted(jnp.cumsum(tallies), jnp.arange(rows * top), side="right").astype(jnp.int32)
    table = items.reshape(top, rows).T
    table = table[jax.random.permutation(jax.random.fold_in(own, 1), rows)]
    turn = jax.random.randint(jax.random.fold_in(own, 2), (rows, 1), 0, top)
    return jnp.take_along_axis(table, (jnp.arange(top)[None, :] + turn) % top, axis=1)


def load_shares(amount, total, reach, slope, full):
    loads = [(1 << 20) // math.isqrt(grade ** slope) + 1 for grade in range(1, amount + 1)]
    largest = reach if full else min(reach, max(-(-total // amount), total * loads[0] // sum(loads)))
    least = 1 if total - largest >= amount - 1 else 0
    given, rest = [largest] + [least] * (amount - 1), total - largest - least * (amount - 1)
    while rest > 0:
        free = [i for i in range(1, amount) if given[i] < largest] or [i for i in range(1, amount) if given[i] < reach]
        pool, left = sum([loads[i] for i in free]), rest
        for i in free:
            addition = min(reach - given[i], max(1, left * loads[i] // pool), rest)
            given[i] = given[i] + addition
            rest = rest - addition
    return np.array(given)


def scatter_about(own_key, extent, scale, limit, shards=(), held_as=jnp.bfloat16):
    entries = scale * jax.random.normal(own_key, extent, jnp.float32)
    if shards:
        entries = entries * steps_of(own_key, extent, shards, -0.22, 0.18)
    return jnp.clip(entries, -limit, limit).astype(held_as)


def setup_inputs(seed: int = 0) -> dict:
    key_of = jax.random.split(jax.random.key(seed), 8)
    tokens = scatter_about(key_of[0], (TOKENS, D), 1.0, 6.0, ((0, 64),))
    cotangent = scatter_about(key_of[1], (TOKENS, D), 1.0, 6.0, ((0, 64),))
    routes_keys = jax.random.split(jax.random.fold_in(key_of[2], 1), TOKENS // TOK_DEV)
    routes_turns = jax.random.permutation(jax.random.fold_in(key_of[2], 3), TOKENS // TOK_DEV)
    routes = jax.vmap(lambda own, number: routed_block(jax.random.fold_in(key_of[2], 2), own, number, TOK_DEV, EXPERTS, TOP, CAP, 2))(routes_keys, routes_turns).reshape((TOKENS, TOP))
    gate_weights = jnp.clip(0.2 + 0.8 * jax.random.uniform(key_of[3], (TOKENS, TOP), jnp.float32) ** steps_of(key_of[3], (TOKENS, TOP), ((0, 64),), -0.2, 0.2), 0.2, 1.0)
    w_gate = scatter_about(key_of[4], (EXPERTS, D, FF), D ** -0.5, 0.125, ((0, 64), (2, 4)))
    w_up = scatter_about(key_of[5], (EXPERTS, D, FF), D ** -0.5, 0.125, ((0, 64), (2, 4)))
    w_down = scatter_about(key_of[6], (EXPERTS, FF, D), FF ** -0.5, 0.125, ((0, 64), (1, 4)))
    return dict(tokens=tokens, cotangent=cotangent, routes=routes, gate_weights=gate_weights, w_gate=w_gate, w_up=w_up, w_down=w_down)


def place(block_routes, experts, capacity):
    flat = block_routes.reshape(-1).astype(jnp.int32)
    onehot = (flat[:, None] == jnp.arange(experts, dtype=jnp.int32)[None, :]).astype(jnp.int32)
    before = jnp.cumsum(onehot, axis=0) - onehot
    position = jnp.sum(before * onehot, axis=1).astype(jnp.int32)
    return (flat * capacity + position).astype(jnp.int32)


def reference(tokens, cotangent, routes, gate_weights, w_gate, w_up, w_down):
    items = TOKENS * TOP
    slot_index = jax.vmap(lambda block: place(block, EXPERTS, CAP))(routes.reshape(N_EP, TOK_DEV * TOP))
    item_ids = jnp.arange(items, dtype=jnp.int32).reshape(N_EP, TOK_DEV * TOP)
    empty = jnp.full((N_EP, EXPERTS * CAP), items, jnp.int32)
    table = jax.vmap(lambda base, where, ids: base.at[where].set(ids))(empty, slot_index, item_ids)
    table = table.reshape(N_EP, EXPERTS, CAP).transpose(1, 0, 2).reshape(EXPERTS, N_EP * CAP)
    tokens_pad = jnp.concatenate([tokens, jnp.zeros((1, D), tokens.dtype)], axis=0)
    cot_pad = jnp.concatenate([cotangent, jnp.zeros((1, D), cotangent.dtype)], axis=0)
    gates_pad = jnp.concatenate([gate_weights.reshape(-1), jnp.zeros((1,), jnp.float32)])
    gates_low = lax.optimization_barrier(gates_pad.astype(jnp.bfloat16)).astype(jnp.float32)
    group = FF // N_TP

    def expert_step(carry, inputs):
        grad_acc, score_acc = carry
        item, wg, wu, wd = inputs
        row = (item // TOP).astype(jnp.int32)
        x_rows = tokens_pad[row]
        c_rows = cot_pad[row]
        scale = gates_low[item][:, None]
        pre_gate = jnp.dot(x_rows, wg, preferred_element_type=jnp.float32)
        pre_up = jnp.dot(x_rows, wu, preferred_element_type=jnp.float32)
        sig = jax.nn.sigmoid(pre_gate)
        act = pre_gate * sig
        hidden = (act * pre_up).astype(jnp.bfloat16)
        back = jnp.dot(c_rows, wd.T, preferred_element_type=jnp.float32)
        scaled = scale * back
        d_out = (scale * c_rows.astype(jnp.float32)).astype(jnp.bfloat16)
        d_gate_pre = (scaled * pre_up * sig * (1.0 + pre_gate * (1.0 - sig))).astype(jnp.bfloat16)
        d_up_pre = (scaled * act).astype(jnp.bfloat16)
        grad_down = jnp.dot(hidden.T, d_out, preferred_element_type=jnp.float32).astype(jnp.bfloat16)
        grad_gate = jnp.dot(x_rows.T, d_gate_pre, preferred_element_type=jnp.float32).astype(jnp.bfloat16)
        grad_up = jnp.dot(x_rows.T, d_up_pre, preferred_element_type=jnp.float32).astype(jnp.bfloat16)
        route_grad = jnp.zeros((x_rows.shape[0], D), jnp.float32)
        route_score = jnp.zeros((x_rows.shape[0],), jnp.float32)
        hidden_wide = hidden.astype(jnp.float32)
        for j in range(N_TP):
            lo = j * group
            hi = lo + group
            piece = jnp.dot(d_gate_pre[:, lo:hi], wg[:, lo:hi].T, preferred_element_type=jnp.float32)
            piece = piece + jnp.dot(d_up_pre[:, lo:hi], wu[:, lo:hi].T, preferred_element_type=jnp.float32)
            route_grad = route_grad + piece.astype(jnp.bfloat16).astype(jnp.float32)
            partial_score = jnp.sum(hidden_wide[:, lo:hi] * back[:, lo:hi], axis=1)
            route_score = route_score + partial_score.astype(jnp.bfloat16).astype(jnp.float32)
        route_grad = route_grad.astype(jnp.bfloat16).astype(jnp.float32)
        route_score = route_score.astype(jnp.bfloat16).astype(jnp.float32)
        grad_acc = grad_acc.at[row].add(route_grad)
        score_acc = score_acc.at[item].add(route_score)
        gate_wide = grad_gate.astype(jnp.float32)
        up_wide = grad_up.astype(jnp.float32)
        norms = jnp.sum(gate_wide * gate_wide + up_wide * up_wide, axis=1)
        return (grad_acc, score_acc), (grad_gate, grad_up, grad_down, norms)

    start = (jnp.zeros((TOKENS + 1, D), jnp.float32), jnp.zeros((items + 1,), jnp.float32))
    (grad_acc, score_acc), (gate_grad, up_grad, down_grad, norms) = lax.scan(
        expert_step, start, (table, w_gate, w_up, w_down))
    token_grad = grad_acc[:TOKENS].astype(jnp.bfloat16)
    score_grad = score_acc[:items].reshape(TOKENS, TOP)
    return token_grad, score_grad, gate_grad, up_grad, down_grad, jnp.sum(norms, axis=0)
```

```python
import jax
import jax.numpy as jnp
from jax import lax
from jax.experimental import pallas as pl
from jax.experimental.pallas import tpu as pltpu
from jax.sharding import PartitionSpec as P


BF = jnp.bfloat16
F32 = jnp.float32
PAD = 16

NT = (((1,), (1,)), ((), ()))
TN = (((0,), (0,)), ((), ()))


def iota(shape, dim):
    return lax.broadcasted_iota(jnp.int32, shape, dim)


def dot(a, b, dims=(((1,), (0,)), ((), ()))):
    return lax.dot_general(a, b, dims, preferred_element_type=F32)


def one_hots(routes, experts):
    toks = routes.shape[1]
    ids = iota((experts, toks), 0)
    hot = [jnp.where(routes[k : k + 1, :] == ids, 1.0, 0.0) for k in range(2)]
    both = (hot[0] + hot[1]).astype(BF)
    upper = jnp.where(iota((toks, toks), 0) < iota((toks, toks), 1), 1.0, 0.0).astype(BF)
    before = dot(both, upper)
    pos = [jnp.sum(h * before, axis=0, keepdims=True).astype(jnp.int32) for h in hot]
    return hot, pos


def selector(routes, pos, rows):
    toks = routes.shape[1]
    at = iota((rows, toks), 0)
    sel = jnp.zeros((rows, toks), F32)
    for k in range(2):
        sel = sel + jnp.where(routes[k : k + 1, :] * PAD + pos[k] == at, 1.0, 0.0)
    return sel.astype(BF)


def spare_rows(rows, experts, cap):
    return jnp.where(iota((rows, experts), 0) == iota((rows, experts), 1) * PAD + cap, 1.0, 0.0).astype(BF)


def dispatch_kernel(cap, experts, tp_ref, routes_ref, gates_ref, tok_ref, cot_ref, x_ref, c_ref):
    routes = routes_ref[...]
    gates = gates_ref[...].astype(BF).astype(F32)
    rows = experts * PAD
    hot, pos = one_hots(routes, experts)
    sel = selector(routes, pos, rows)
    x_ref[...] = dot(sel, tok_ref[...]).astype(BF)
    width = cot_ref.shape[1]
    toks = routes.shape[1]
    table = jnp.zeros((experts, width), F32)
    for k in range(2):
        own = (hot[k] * gates[k : k + 1, :]).astype(BF)
        lane = jnp.where(iota((width, toks), 0) == pos[k], 1.0, 0.0).astype(BF)
        table = table + dot(own, lane, NT)
    c_ref[...] = (dot(sel, cot_ref[...]) + dot(spare_rows(rows, experts, cap), table.astype(BF))).astype(BF)


def dispatch(tp, routes_t, gates_t, tokens, cotangent, cap, experts, quarter):
    rows = experts * PAD
    toks = tokens.shape[0]
    return pl.pallas_call(
        lambda *refs: dispatch_kernel(cap, experts, *refs),
        grid_spec=pltpu.PrefetchScalarGridSpec(
            num_scalar_prefetch=1,
            grid=(1,),
            in_specs=[
                pl.BlockSpec((2, toks), lambda i, s: (0, 0)),
                pl.BlockSpec((2, toks), lambda i, s: (0, 0)),
                pl.BlockSpec((toks, quarter), lambda i, s: (0, s[0])),
                pl.BlockSpec((toks, quarter), lambda i, s: (0, s[0])),
            ],
            out_specs=[pl.BlockSpec((rows, quarter), lambda i, s: (0, 0))] * 2,
        ),
        out_shape=[jax.ShapeDtypeStruct((rows, quarter), BF)] * 2,
        name="dispatch",
    )(tp, routes_t, gates_t, tokens, cotangent)


def combine_kernel(cap, experts, routes_ref, *refs):
    *ret_refs, tok_ref, score_ref = refs
    routes = routes_ref[...]
    rows = experts * PAD
    hot, pos = one_hots(routes, experts)
    sel = selector(routes, pos, rows)
    at = 0
    for ret_ref in ret_refs:
        n = ret_ref.shape[1]
        tok_ref[:, at : at + n] = dot(sel, ret_ref[...], TN).astype(BF)
        at += n
    table = dot(spare_rows(rows, experts, cap), ret_refs[0][:, :128], TN).astype(BF)
    out = []
    for k in range(2):
        column = dot(table, hot[k].astype(BF), TN)
        lane = jnp.where(iota(column.shape, 0) == pos[k], 1.0, 0.0)
        out.append(jnp.sum(column * lane, axis=0, keepdims=True))
    score_ref[...] = jnp.concatenate(out, axis=0)


def combine(routes_t, rets, cap, experts):
    toks = routes_t.shape[1]
    return pl.pallas_call(
        lambda *refs: combine_kernel(cap, experts, *refs),
        out_shape=[
            jax.ShapeDtypeStruct((toks, sum(r.shape[1] for r in rets)), BF),
            jax.ShapeDtypeStruct((2, toks), F32),
        ],
        name="combine",
    )(routes_t, *rets)


def compact_kernel(cap, in_ref, *out_refs):
    full, part = 8 * PAD, 8 * cap
    row, col = iota((part, full), 0), iota((part, full), 1)
    sel = jnp.where(row // cap * PAD + row % cap == col, 1.0, 0.0).astype(BF)
    for b in range(in_ref.shape[0] // full):
        got = dot(sel, in_ref[b * full : (b + 1) * full, :]).astype(BF)
        at = 0
        for out_ref in out_refs:
            n = out_ref.shape[1]
            out_ref[b * part : (b + 1) * part, :] = got[:, at : at + n]
            at += n


def compact(groups16, cap, parts):
    groups, _, width = groups16.shape
    return pl.pallas_call(
        lambda *refs: compact_kernel(cap, *refs),
        out_shape=[jax.ShapeDtypeStruct((groups * cap, width // parts), BF)] * parts,
        name="compact",
    )(groups16.reshape(groups * PAD, width))


def expand_kernel(cap, parts, score_ref, *refs):
    out_ref = refs[-1]
    full, part = 8 * PAD, 8 * cap
    row, col = iota((full, part), 0), iota((full, part), 1)
    sel = jnp.where((row % PAD < cap) & (row // PAD * cap + row % PAD == col), 1.0, 0.0).astype(BF)
    spare = spare_rows(full, 8, cap)
    n = out_ref.shape[1] // parts
    for b in range(out_ref.shape[0] // full):
        for h in range(parts):
            terms = [r[b * part : (b + 1) * part, :].astype(F32) for r in refs[3 * h : 3 * h + 3]]
            mine = (terms[0] + terms[1] + terms[2]).astype(BF)
            got = dot(sel, mine)
            if h == 0:
                got = got + dot(spare, score_ref[b * 8 : (b + 1) * 8, :])
            out_ref[b * full : (b + 1) * full, h * n : (h + 1) * n] = got.astype(BF)


def expand(scores, terms, cap, experts):
    flat = [t for part in terms for t in part]
    n = flat[0].shape[1]
    return pl.pallas_call(
        lambda *refs: expand_kernel(cap, len(terms), *refs),
        out_shape=jax.ShapeDtypeStruct((experts * PAD, n * len(terms)), BF),
        name="expand",
    )(scores, *flat)


def sum_over(value, axis, flips):
    size = lax.axis_size(axis)
    for flip in flips:
        value = value + lax.ppermute(value, axis, [(i, i ^ flip) for i in range(size)])
    return value


def after(value, first):
    return lax.optimization_barrier((value, first))[0]


def on_device(tokens, cotangent, routes, gate_weights, w_gate, w_up, w_down):
    experts = lax.axis_size("ep")
    groups = lax.axis_size("tp")
    tok_rows, width = tokens.shape
    cap = 2 * tok_rows * routes.shape[1] // experts
    slots = experts * cap
    quarter = width // groups
    cw = quarter // 2
    tp = lax.axis_index("tp")
    up = [(i, (i + 1) % groups) for i in range(groups)]
    down = [(i, (i - 1) % groups) for i in range(groups)]
    place = [((tp + shift) & (groups - 1)) * quarter for shift in range(groups)]
    routes_t = routes.T
    x_send, c_send = dispatch(
        tp.reshape(1), routes_t, gate_weights.T, tokens, cotangent, cap, experts, quarter
    )

    def exchange(rows):
        return lax.all_to_all(
            rows.reshape(experts, PAD, -1), "ep", split_axis=0, concat_axis=0, tiled=True
        )

    def gather(owns):
        o0, o1 = owns
        l0, r1 = lax.ppermute(o0, "tp", up), lax.ppermute(o1, "tp", down)
        l1, r0 = lax.ppermute(o1, "tp", up), lax.ppermute(o0, "tp", down)
        f0, f1 = lax.ppermute(l0, "tp", up), lax.ppermute(r1, "tp", down)
        full = jnp.zeros((slots, width), BF)
        for shift, pair in ((0, (o0, o1)), (3, (l0, l1)), (1, (r0, r1)), (2, (f0, f1))):
            for h, piece in enumerate(pair):
                full = lax.dynamic_update_slice(full, piece, (0, place[shift] + h * cw))
        return full

    x_got = exchange(x_send)
    c_send = after(c_send, x_got)
    c_got = exchange(c_send)
    x_rows = gather(compact(x_got, cap, 2))
    scale = c_got[:, cap, :cap].reshape(slots, 1).astype(F32)
    wg = w_gate[0]
    wu = w_up[0]
    wd = w_down[0]
    c_own = compact(c_got, cap, 2)
    pre_gate = dot(x_rows, wg)
    pre_up = dot(x_rows, wu)
    c_rows = gather(c_own)
    sig = jax.nn.sigmoid(pre_gate)
    act = pre_gate * sig
    hidden = (act * pre_up).astype(BF)
    back = dot(c_rows, wd, NT)
    score_part = jnp.sum(hidden.astype(F32) * back, axis=1)
    scaled = scale * back
    d_gate = (scaled * pre_up * sig * (1.0 + pre_gate * (1.0 - sig))).astype(BF)
    d_up = (scaled * act).astype(BF)

    def piece(shift, h):
        g = lax.dynamic_slice_in_dim(wg, place[shift] + h * cw, cw, 0)
        u = lax.dynamic_slice_in_dim(wu, place[shift] + h * cw, cw, 0)
        return dot(d_gate, g, NT) + dot(d_up, u, NT)

    p20, p21 = piece(2, 0).astype(BF), piece(2, 1).astype(BF)
    f0, f1 = lax.ppermute(p20, "tp", up), lax.ppermute(p21, "tp", down)
    p30, p11 = piece(3, 0).astype(BF), piece(1, 1).astype(BF)
    l0, r1 = lax.ppermute(p30, "tp", down), lax.ppermute(p11, "tp", up)
    p10, p31 = piece(1, 0), piece(3, 1)
    r0 = lax.ppermute((p10 + f0.astype(F32)).astype(BF), "tp", up)
    l1 = lax.ppermute((p31 + f1.astype(F32)).astype(BF), "tp", down)
    p00, p01 = piece(0, 0), piece(0, 1)

    own_score = score_part.astype(BF).astype(F32).reshape(experts, cap)
    scores = sum_over(own_score, "tp", (2, 1)).astype(BF)
    scores = jnp.pad(scores, ((0, 0), (0, cw - cap)))
    block = expand(scores, [(p00, l0, r0), (p01, l1, r1)], cap, experts)
    ret = exchange(block).reshape(experts * PAD, quarter)

    d_gate, d_up, hidden_w = after((d_gate, d_up, hidden), (p20, p21, p30, p11, p10, p31))
    d_out = (scale * c_rows).astype(BF)
    grad_gate = dot(x_rows, d_gate, TN).astype(BF)
    grad_up = dot(x_rows, d_up, TN).astype(BF)
    grad_down = dot(hidden_w, d_out, TN).astype(BF)
    gate_wide = grad_gate.astype(F32)
    up_wide = grad_up.astype(F32)
    norm_part = jnp.sum(gate_wide * gate_wide + up_wide * up_wide, axis=1)
    row_norms = sum_over(norm_part, "tp", (2, 1))
    row_norms = sum_over(row_norms, "ep", [1 << b for b in range(experts.bit_length() - 1)])

    token_grad, score_t = combine(routes_t, [ret], cap, experts)
    return (token_grad, score_t.T, grad_gate[None], grad_up[None], grad_down[None], row_norms)


def solution(mesh):
    return jax.shard_map(
        on_device,
        mesh=mesh,
        in_specs=(
            P("ep", None),
            P("ep", None),
            P("ep", None),
            P("ep", None),
            P("ep", None, "tp"),
            P("ep", None, "tp"),
            P("ep", "tp", None),
        ),
        out_specs=(
            P("ep", "tp"),
            P("ep", None),
            P("ep", None, "tp"),
            P("ep", None, "tp"),
            P("ep", "tp", None),
            P(),
        ),
        check_vma=False,
    )
```

```python
import jax
import jax.numpy as jnp
from jax import lax
from jax.experimental import pallas as pl
from jax.experimental.pallas import tpu as pltpu
from jax.sharding import PartitionSpec as P


BF = jnp.bfloat16
F32 = jnp.float32
PAD = 16

NT = (((1,), (1,)), ((), ()))
TN = (((0,), (0,)), ((), ()))


def iota(shape, dim):
    return lax.broadcasted_iota(jnp.int32, shape, dim)


def dot(a, b, dims=(((1,), (0,)), ((), ()))):
    return lax.dot_general(a, b, dims, preferred_element_type=F32)


def one_hots(routes, experts):
    toks = routes.shape[1]
    ids = iota((experts, toks), 0)
    hot = [jnp.where(routes[k : k + 1, :] == ids, 1.0, 0.0) for k in range(2)]
    both = (hot[0] + hot[1]).astype(BF)
    upper = jnp.where(iota((toks, toks), 0) < iota((toks, toks), 1), 1.0, 0.0).astype(BF)
    before = dot(both, upper)
    pos = [jnp.sum(h * before, axis=0, keepdims=True).astype(jnp.int32) for h in hot]
    return hot, pos


def selector(routes, pos, rows):
    toks = routes.shape[1]
    at = iota((rows, toks), 0)
    sel = jnp.zeros((rows, toks), F32)
    for k in range(2):
        sel = sel + jnp.where(routes[k : k + 1, :] * PAD + pos[k] == at, 1.0, 0.0)
    return sel.astype(BF)


def spare_rows(rows, experts, cap):
    return jnp.where(iota((rows, experts), 0) == iota((rows, experts), 1) * PAD + cap, 1.0, 0.0).astype(BF)


def dispatch_kernel(cap, experts, tp_ref, routes_ref, gates_ref, tok_ref, cot_ref, x_ref, c_ref):
    routes = routes_ref[...]
    gates = gates_ref[...].astype(BF).astype(F32)
    rows = experts * PAD
    hot, pos = one_hots(routes, experts)
    sel = selector(routes, pos, rows)
    x_ref[...] = dot(sel, tok_ref[...]).astype(BF)
    width = cot_ref.shape[1]
    toks = routes.shape[1]
    table = jnp.zeros((experts, width), F32)
    for k in range(2):
        own = (hot[k] * gates[k : k + 1, :]).astype(BF)
        lane = jnp.where(iota((width, toks), 0) == pos[k], 1.0, 0.0).astype(BF)
        table = table + dot(own, lane, NT)
    c_ref[...] = (dot(sel, cot_ref[...]) + dot(spare_rows(rows, experts, cap), table.astype(BF))).astype(BF)


def dispatch(tp, routes_t, gates_t, tokens, cotangent, cap, experts, quarter):
    rows = experts * PAD
    toks = tokens.shape[0]
    return pl.pallas_call(
        lambda *refs: dispatch_kernel(cap, experts, *refs),
        grid_spec=pltpu.PrefetchScalarGridSpec(
            num_scalar_prefetch=1,
            grid=(1,),
            in_specs=[
                pl.BlockSpec((2, toks), lambda i, s: (0, 0)),
                pl.BlockSpec((2, toks), lambda i, s: (0, 0)),
                pl.BlockSpec((toks, quarter), lambda i, s: (0, s[0])),
                pl.BlockSpec((toks, quarter), lambda i, s: (0, s[0])),
            ],
            out_specs=[pl.BlockSpec((rows, quarter), lambda i, s: (0, 0))] * 2,
        ),
        out_shape=[jax.ShapeDtypeStruct((rows, quarter), BF)] * 2,
        name="dispatch",
    )(tp, routes_t, gates_t, tokens, cotangent)


def combine_kernel(cap, experts, routes_ref, *refs):
    *ret_refs, tok_ref, score_ref = refs
    routes = routes_ref[...]
    rows = experts * PAD
    hot, pos = one_hots(routes, experts)
    sel = selector(routes, pos, rows)
    at = 0
    for ret_ref in ret_refs:
        n = ret_ref.shape[1]
        tok_ref[:, at : at + n] = dot(sel, ret_ref[...], TN).astype(BF)
        at += n
    table = dot(spare_rows(rows, experts, cap), ret_refs[0][:, :128], TN).astype(BF)
    out = []
    for k in range(2):
        column = dot(table, hot[k].astype(BF), TN)
        lane = jnp.where(iota(column.shape, 0) == pos[k], 1.0, 0.0)
        out.append(jnp.sum(column * lane, axis=0, keepdims=True))
    score_ref[...] = jnp.concatenate(out, axis=0)


def combine(routes_t, rets, cap, experts):
    toks = routes_t.shape[1]
    return pl.pallas_call(
        lambda *refs: combine_kernel(cap, experts, *refs),
        out_shape=[
            jax.ShapeDtypeStruct((toks, sum(r.shape[1] for r in rets)), BF),
            jax.ShapeDtypeStruct((2, toks), F32),
        ],
        name="combine",
    )(routes_t, *rets)


def compact_kernel(cap, in_ref, *out_refs):
    full, part = 8 * PAD, 8 * cap
    row, col = iota((part, full), 0), iota((part, full), 1)
    sel = jnp.where(row // cap * PAD + row % cap == col, 1.0, 0.0).astype(BF)
    for b in range(in_ref.shape[0] // full):
        got = dot(sel, in_ref[b * full : (b + 1) * full, :]).astype(BF)
        at = 0
        for out_ref in out_refs:
            n = out_ref.shape[1]
            out_ref[b * part : (b + 1) * part, :] = got[:, at : at + n]
            at += n


def compact(groups16, cap, parts):
    groups, _, width = groups16.shape
    return pl.pallas_call(
        lambda *refs: compact_kernel(cap, *refs),
        out_shape=[jax.ShapeDtypeStruct((groups * cap, width // parts), BF)] * parts,
        name="compact",
    )(groups16.reshape(groups * PAD, width))


def expand_kernel(cap, parts, score_ref, *refs):
    out_ref = refs[-1]
    full, part = 8 * PAD, 8 * cap
    row, col = iota((full, part), 0), iota((full, part), 1)
    sel = jnp.where((row % PAD < cap) & (row // PAD * cap + row % PAD == col), 1.0, 0.0).astype(BF)
    spare = spare_rows(full, 8, cap)
    n = out_ref.shape[1] // parts
    for b in range(out_ref.shape[0] // full):
        for h in range(parts):
            terms = [r[b * part : (b + 1) * part, :].astype(F32) for r in refs[3 * h : 3 * h + 3]]
            mine = (terms[0] + terms[1] + terms[2]).astype(BF)
            got = dot(sel, mine)
            if h == 0:
                got = got + dot(spare, score_ref[b * 8 : (b + 1) * 8, :])
            out_ref[b * full : (b + 1) * full, h * n : (h + 1) * n] = got.astype(BF)


def expand(scores, terms, cap, experts):
    flat = [t for part in terms for t in part]
    n = flat[0].shape[1]
    return pl.pallas_call(
        lambda *refs: expand_kernel(cap, len(terms), *refs),
        out_shape=jax.ShapeDtypeStruct((experts * PAD, n * len(terms)), BF),
        name="expand",
    )(scores, *flat)


def weight_grad_kernel(norms, scaled, *refs):
    if scaled:
        scale_ref, *refs = refs
    rows_ref, *refs = refs
    *refs, all_ref = refs
    count = (len(refs) - (1 if norms else 0)) // 2
    units = refs[0].shape[0]

    @pl.when(pl.program_id(0) == 0)
    def _():
        for i, d_ref in enumerate(refs[:count]):
            all_ref[i * units : (i + 1) * units, :] = d_ref[...]

    rows = rows_ref[...]
    if scaled:
        rows = (scale_ref[...] * rows.astype(F32)).astype(BF)
    total = 0.0
    grads = dot(all_ref[...], rows).astype(BF)
    for i, out_ref in enumerate(refs[count : 2 * count]):
        grad = grads[i * units : (i + 1) * units]
        out_ref[...] = grad
        wide = grad.astype(F32)
        if norms:
            total = total + jnp.sum(wide * wide, axis=0, keepdims=True)
    if norms:
        refs[-1][...] = total


def weight_grads(rows, ds, scale=None, norms=False, block=512):
    slots, width = rows.shape
    units = ds[0].shape[0]
    by_col = lambda n: pl.BlockSpec((n, block), lambda i: (0, i))
    whole = lambda a: pl.BlockSpec(a.shape, lambda i: (0, 0))
    extra = [] if scale is None else [scale]
    outs = [jax.ShapeDtypeStruct((units, width), BF)] * len(ds)
    if norms:
        outs.append(jax.ShapeDtypeStruct((1, width), F32))
    return pl.pallas_call(
        lambda *refs: weight_grad_kernel(norms, scale is not None, *refs),
        grid=(width // block,),
        in_specs=[whole(a) for a in extra] + [by_col(slots)] + [whole(d) for d in ds],
        out_specs=[by_col(o.shape[0]) for o in outs],
        out_shape=outs,
        scratch_shapes=[pltpu.VMEM((len(ds) * units, slots), BF)],
        cost_estimate=pl.CostEstimate(
            flops=2 * len(ds) * slots * units * width, bytes_accessed=8 * 2**20, transcendentals=0
        ),
    )(*extra, rows, *ds)


def sum_over(value, axis, flips):
    size = lax.axis_size(axis)
    for a, b in flips:
        other = [
            lax.ppermute(value, axis, [(i, i ^ flip) for i in range(size)]) for flip in (a, b, a ^ b)
        ]
        value = (value + other[0]) + (other[1] + other[2])
    return value


def after(value, first):
    return lax.optimization_barrier((value, first))[0]


def on_device(tokens, cotangent, routes, gate_weights, w_gate, w_up, w_down):
    experts = lax.axis_size("ep")
    groups = lax.axis_size("tp")
    tok_rows, width = tokens.shape
    cap = 2 * tok_rows * routes.shape[1] // experts
    slots = experts * cap
    quarter = width // groups
    cw = quarter // 2
    tp = lax.axis_index("tp")
    up = [(i, (i + 1) % groups) for i in range(groups)]
    down = [(i, (i - 1) % groups) for i in range(groups)]
    place = [((tp + shift) & (groups - 1)) * quarter for shift in range(groups)]
    routes_t = routes.T
    x_send, c_send = dispatch(
        tp.reshape(1), routes_t, gate_weights.T, tokens, cotangent, cap, experts, quarter
    )

    def exchange(rows):
        return lax.all_to_all(
            rows.reshape(experts, PAD, -1), "ep", split_axis=0, concat_axis=0, tiled=True
        )

    def gather(owns, first=None):
        o0, o1 = owns
        l0, r1 = lax.ppermute(o0, "tp", up), lax.ppermute(o1, "tp", down)
        l1, r0 = lax.ppermute(o1, "tp", up), lax.ppermute(o0, "tp", down)
        f0, f1 = lax.ppermute(l0, "tp", up), lax.ppermute(r1, "tp", down)
        full = jnp.zeros((slots, width), BF)
        for shift, pair in ((0, (o0, o1)), (3, (l0, l1)), (1, (r0, r1)), (2, (f0, f1))):
            if shift == 2 and first is not None:
                full = after(full, first)
            for h, piece in enumerate(pair):
                full = lax.dynamic_update_slice(full, piece, (0, place[shift] + h * cw))
        return full

    x_got = exchange(x_send)
    c_send = after(c_send, x_got)
    c_got = exchange(c_send)
    c_own = compact(c_got, cap, 2)
    x_rows = gather(compact(x_got, cap, 2), c_own)
    wg = w_gate[0]
    wu = w_up[0]
    wd = w_down[0]
    pre_gate = dot(x_rows, wg)
    pre_up = dot(after(x_rows, pre_gate), wu)
    scale = c_got[:, cap, :cap].reshape(slots, 1).astype(F32)
    c_rows = gather(c_own)
    sig = jax.nn.sigmoid(pre_gate)
    act = pre_gate * sig
    hidden = (act * pre_up).astype(BF)
    back = dot(c_rows, wd, NT)
    score_part = jnp.sum(hidden.astype(F32) * back, axis=1)
    scaled = scale * back
    d_gate = (scaled * pre_up * sig * (1.0 + pre_gate * (1.0 - sig))).astype(BF)
    d_up = (scaled * act).astype(BF)

    def piece(d, at, size):
        g = lax.dynamic_slice_in_dim(wg, at, size, 0)
        u = lax.dynamic_slice_in_dim(wu, at, size, 0)
        return (dot(d[0], g, NT) + dot(d[1], u, NT)).astype(BF)

    d = (d_gate, d_up)
    far = [piece(d, place[2] + h * cw, cw) for h in range(2)]
    f0, f1 = lax.ppermute(far[0], "tp", up), lax.ppermute(far[1], "tp", down)
    own_score = after(score_part.astype(BF).astype(F32).reshape(experts, cap), far)
    scores = sum_over(own_score, "tp", ((1, 2),))
    scores = jnp.pad(scores.astype(BF), ((0, 0), (0, quarter - cap)))
    d = after(d, far)
    right, left = piece(d, place[1], quarter), piece(d, place[3], quarter)
    f0 = jnp.pad(after(f0, (right, left)), ((0, 0), (0, cw)))
    f1 = jnp.pad(after(f1, (right, left)), ((0, 0), (cw, 0)))
    right = (right.astype(F32) + f0.astype(F32)).astype(BF)
    left = (left.astype(F32) + f1.astype(F32)).astype(BF)
    d = after(d, (right, left))
    from_left = lax.ppermute(right, "tp", up)
    from_right = lax.ppermute(left, "tp", down)
    grad_gate, grad_up, norm_part = weight_grads(x_rows, (d[0].T, d[1].T), norms=True)
    own = piece(after(d, norm_part), place[0], quarter)
    block = expand(scores, [(own, from_left, from_right)], cap, experts)
    ret = exchange(block).reshape(experts * PAD, quarter)

    (grad_down,) = weight_grads(c_rows, (hidden.T,), scale=scale)
    row_norms = sum_over(norm_part, "ep", ((16, 32),))
    row_norms = sum_over(row_norms, "ep", ((1, 8),))
    row_norms = sum_over(row_norms, "ep", ((2, 4),))
    row_norms = sum_over(row_norms, "tp", ((1, 2),))[0]

    token_grad, score_t = combine(routes_t, [ret], cap, experts)
    return (token_grad, score_t.T, grad_gate.T[None], grad_up.T[None], grad_down[None], row_norms)


def solution(mesh):
    return jax.shard_map(
        on_device,
        mesh=mesh,
        in_specs=(
            P("ep", None),
            P("ep", None),
            P("ep", None),
            P("ep", None),
            P("ep", None, "tp"),
            P("ep", None, "tp"),
            P("ep", "tp", None),
        ),
        out_specs=(
            P("ep", "tp"),
            P("ep", None),
            P("ep", None, "tp"),
            P("ep", None, "tp"),
            P("ep", "tp", None),
            P(),
        ),
        check_vma=False,
    )
```
